32 devices in a mesh: ep: 8 (over z, core), tp: 4 (over y, x).
Axes of the slice: x: 2, y: 2, z: 4, core: 2. Of those that a mesh axis runs over, the one named last changes fastest.
Arguments:
- tokens: bfloat16 [1024, 2048], P('ep'), may hold values from -6 to 6
- selected: int32 [8, 256], P(None, 'ep'), may hold values from -1 to 127, as said below
- affinity: float32 [8, 256], P(None, 'ep'), may hold values from 0.05 to 1
- w_gate: bfloat16 [8, 2048, 2048], P('ep', None, 'tp'), may hold values from -0.125 to 0.125
- w_up: bfloat16 [8, 2048, 2048], P('ep', None, 'tp'), may hold values from -0.125 to 0.125
- w_down: bfloat16 [8, 2048, 2048], P('ep', 'tp'), may hold values from -0.125 to 0.125
Outputs:
- combined: bfloat16 [1024, 2048], P('ep', 'tp')
The draws below stay inside these ranges and needn't reach their ends.
Inputs may be any that keep to these rules, and one draw needn't show every extreme that they name: `selected`: row e holds 8 aligned groups of 32 entries; the live entries of group j are distinct positions within the j-th block of 128 tokens, stand at the front of the group and are followed by -1; each row has 128 live entries in all, the number in a group varies, and some group of every row is full.
All inputs are finite; a program needn't handle non-finite values.
Results may differ from the reference program's by a relative error of at most 0.015.
Values may be sent and summed in bfloat16 or wider, within the bound.
A program may use at most 64 MiB of HBM per device.

```python
import math
import jax
import jax.numpy as jnp
from jax import lax

D = 2048
FF = 2048
TOK_DEV = 128
EXPERTS = 8
TOKENS = 1024
PICK = 16
MOST = 32
SLOTS = 256
N_EP = 8
N_TP = 4


def draw_selected(key, part):
    half = N_EP // 2
    block_scores = jax.random.randint(jax.random.fold_in(key, 11), (EXPERTS, N_EP), 0, 2 ** 20)
    block_order = jnp.argsort(block_scores * N_EP + jnp.arange(N_EP, dtype=jnp.int32)[None, :], axis=1, stable=True).astype(jnp.int32)
    inverse = jnp.argsort(block_order, axis=1, stable=True).astype(jnp.int32)
    shifts = jax.random.randint(jax.random.fold_in(key, 12), (EXPERTS, half), -PICK, PICK + 1)
    forced = jax.random.randint(jax.random.fold_in(key, 13), (EXPERTS,), 0, half)
    shifts = jnp.where(jnp.arange(half, dtype=jnp.int32)[None, :] == forced[:, None], PICK, shifts)
    counts_paired = jnp.concatenate([PICK + shifts, PICK - shifts], axis=1)
    counts = jnp.take_along_axis(counts_paired, inverse, axis=1)
    scores = jax.random.randint(jax.random.fold_in(key, 17), (EXPERTS, N_EP, TOK_DEV), 0, 2 ** 20)
    distinct = scores * TOK_DEV + jnp.arange(TOK_DEV, dtype=jnp.int32)[None, None, :]
    order = jnp.argsort(distinct, axis=2, stable=True).astype(jnp.int32)[:, :, :MOST]
    live = jnp.arange(MOST, dtype=jnp.int32)[None, None, :] < counts[:, :, None]
    picked = jnp.where(live, order, -1)
    return picked.reshape(EXPERTS, N_EP * MOST).astype(jnp.int32)


def shard_levels(rng, dims, shards, low, largest):
    loudness = 1.0
    for axis_at, shards_of in shards:
        steps = jax.random.uniform(jax.random.fold_in(jax.random.fold_in(rng, 6), axis_at), (shards_of,), jnp.float32, low / len(shards), largest / len(shards))
        loudness = loudness * jnp.repeat(jnp.exp(steps), dims[axis_at] // shards_of).reshape((-1,) + (1,) * (len(dims) - 1 - axis_at))
    return loudness


def normal_values(stream_key, dims, width, most, pieces=(), kind=jnp.bfloat16):
    values = jax.random.normal(stream_key, dims, jnp.float32) * width
    if len(pieces) > 0:
        values = shard_levels(stream_key, dims, pieces, -0.22, 0.18) * values
    return jnp.clip(values, min=-most, max=most).astype(kind)


def setup_inputs(seed: int = 0) -> dict:
    streams_of = jax.random.split(jax.random.key(seed), 7)
    tokens = normal_values(streams_of[0], (TOKENS, D), 1.0, 6.0, ((0, 8),))
    selected = draw_selected(jax.random.fold_in(streams_of[6], 71), 0)
    affinity = jnp.clip(jnp.exp(math.log(1.0) - 2.9957323 * jax.random.uniform(streams_of[2], (EXPERTS, SLOTS), jnp.float32) ** shard_levels(streams_of[2], (EXPERTS, SLOTS), ((1, 8),), -0.2, 0.2)), 0.05, 1.0)
    w_gate = normal_values(streams_of[3], (EXPERTS, D, FF), D ** -0.5, 0.125, ((0, 8), (2, 4)))
    w_up = normal_values(streams_of[4], (EXPERTS, D, FF), D ** -0.5, 0.125, ((0, 8), (2, 4)))
    w_down = normal_values(streams_of[5], (EXPERTS, FF, D), FF ** -0.5, 0.125, ((0, 8), (1, 4)))
    return {"tokens": tokens, "selected": selected, "affinity": affinity, "w_gate": w_gate, "w_up": w_up, "w_down": w_down}


def reference(tokens, selected, affinity, w_gate, w_up, w_down):
    offsets = (jnp.arange(SLOTS, dtype=jnp.int32) // MOST) * TOK_DEV

    def expert_step(carry, inputs):
        index_row, weight_row, gate_mat, up_mat, down_mat = inputs
        live = index_row >= 0
        position = (jnp.maximum(index_row, 0) + offsets).astype(jnp.int32)
        chosen = tokens[position]
        gate_act = jnp.dot(chosen, gate_mat, preferred_element_type=jnp.float32)
        up_act = jnp.dot(chosen, up_mat, preferred_element_type=jnp.float32)
        hidden = (jax.nn.silu(gate_act) * up_act).astype(jnp.bfloat16)
        blocks = hidden.reshape(SLOTS, N_TP, FF // N_TP).astype(jnp.float32)
        down_blocks = down_mat.reshape(N_TP, FF // N_TP, D).astype(jnp.float32)
        partial_value = jnp.einsum('ckf,kfd->kcd', blocks, down_blocks).astype(jnp.bfloat16)
        expert_out = jnp.sum(partial_value.astype(jnp.float32), axis=0).astype(jnp.bfloat16)
        scaled_weight = jnp.where(live, weight_row, jnp.zeros_like(weight_row))
        carry = carry.at[position].add(scaled_weight[:, None] * expert_out.astype(jnp.float32))
        return carry, None

    initial = jnp.zeros((TOKENS, D), jnp.float32)
    result, unused = lax.scan(expert_step, initial, (selected, affinity, w_gate, w_up, w_down))
    return result.astype(jnp.bfloat16)
```

```python
import functools
import math

import jax
import jax.numpy as jnp
from jax import lax
from jax.experimental import pallas as pl
from jax.experimental.pallas import tpu as pltpu
from jax.sharding import PartitionSpec as P

MESH = pl.DeviceIdType.MESH
F32 = jnp.float32
BF16 = jnp.bfloat16
CHUNK = 256


def side_of(n):
    s = math.isqrt(n)
    while n % s:
        s -= 1
    return s


def kernel(
    n_ep, n_tp, chunks,
    tok_hbm, sel_hbm, aff_hbm, wg_hbm, wu_hbm, wd_hbm, out_ref,
    tok, sel, aff, wgu, wd, onehot, weight_hi, weight_lo, expand, compact,
    cnt_out, cnt_in, z_out, z_in, rows, acc, hid, part_out, part_in, ret_out, ret_in,
    s_in, s_wg, s_wu, s_wd, s_cnt_s, s_cnt_r, s_z_s, s_z_r, s_x_s, s_x_r,
    s_p_s, s_p_r, s_r_s, s_r_r,
):
    ep = lax.axis_index("ep")
    tp = lax.axis_index("tp")
    n_tok, feats = tok.shape
    n_exp, group = sel.shape
    fc = feats // chunks
    live = rows.shape[2]
    hidden = hid.shape[1]

    width = side_of(n_tp)
    height = n_tp // width
    y, x = tp // width, lax.rem(tp, width)
    offsets = [(dy, dx) for dy in range(height) for dx in range(width)][1:]
    near = sorted(offsets, key=lambda o: (o[0] > 0) + (o[1] > 0))
    far = near[::-1]

    def tp_to(o):
        return lax.rem(y + o[0], height) * width + lax.rem(x + o[1], width)

    def tp_from(o):
        return lax.rem(y + height - o[0], height) * width + lax.rem(x + width - o[1], width)

    def tp_sem(o):
        return o[0] * width + o[1]

    ep_order = sorted(range(1, n_ep), key=lambda d: (abs(d - n_ep / 2), d))

    def ep_to(d):
        return lax.rem(ep + d, n_ep)

    def rows_of(i):
        return pl.ds(pl.multiple_of(i * group, group), group)

    load_sel = pltpu.make_async_copy(sel_hbm, sel, s_in.at[0])
    load_tok = pltpu.make_async_copy(
        tok_hbm.at[:, pl.ds(pl.multiple_of(tp * feats, 128), feats)], tok, s_in.at[1]
    )
    load_aff = pltpu.make_async_copy(aff_hbm, aff, s_in.at[2])
    load_sel.start()
    load_tok.start()

    barrier = pltpu.get_barrier_semaphore()
    for d in ep_order:
        pl.semaphore_signal(barrier, inc=1, device_id={"ep": ep_to(d)}, device_id_type=MESH)
    for o in far:
        pl.semaphore_signal(barrier, inc=1, device_id={"tp": tp_to(o)}, device_id_type=MESH)

    load_aff.start()
    load_w = []
    for k in range(n_tp):
        for c in range(chunks):
            at = pl.ds(k * feats + c * fc, fc)
            load_w.append(pltpu.make_async_copy(
                wg_hbm.at[0, at, :], wgu.at[k, c, :, pl.ds(0, hidden)], s_wg.at[k, c]))
            load_w.append(pltpu.make_async_copy(
                wu_hbm.at[0, at, :], wgu.at[k, c, :, pl.ds(hidden, hidden)], s_wu.at[k, c]))
    load_d = [
        pltpu.make_async_copy(
            wd_hbm.at[0, :, pl.ds(k * feats, feats)], wd.at[k], s_wd.at[k])
        for k in range(n_tp)
    ]
    for copy in load_w + load_d:
        copy.start()

    load_sel.wait()
    picked = sel[...].astype(F32)
    count = jnp.sum(jnp.where(picked >= 0, 1.0, 0.0), axis=1, keepdims=True)
    for e in range(n_exp):
        cnt_out[e] = jnp.broadcast_to(count[e:e + 1, :], (8, 128))
    picked_t = jnp.transpose(picked)
    token_lane = lax.broadcasted_iota(jnp.int32, (group, n_tok), 1).astype(F32)
    for e in range(n_exp):
        onehot[pl.ds(e * group, group), :] = jnp.where(
            picked_t[:, e:e + 1] == token_lane, 1.0, 0.0)
    load_tok.wait()
    pick = onehot[...].astype(BF16)
    for c in range(chunks):
        z_out[c] = jnp.dot(
            pick, tok[:, c * fc:(c + 1) * fc], preferred_element_type=F32).astype(BF16)
        z_in[c, rows_of(ep), :] = z_out[c, rows_of(ep), :]
    cnt_in[ep] = cnt_out[ep]

    pl.semaphore_wait(barrier, len(ep_order) + len(far))

    sent = []
    cnt_copy = {}
    z_copy = {}

    def send(src, dst, ss, rs, to):
        copy = pltpu.make_async_remote_copy(
            src_ref=src, dst_ref=dst, send_sem=ss, recv_sem=rs,
            device_id=to, device_id_type=MESH)
        copy.start()
        sent.append(copy)
        return copy

    for c in range(chunks):
        for d in ep_order:
            z_copy[c, d] = send(
                z_out.at[c, rows_of(ep_to(d)), :], z_in.at[c, rows_of(ep), :],
                s_z_s.at[c, d], s_z_r.at[c, d], {"ep": ep_to(d)})
            if c == 0:
                cnt_copy[d] = send(
                    cnt_out.at[ep_to(d)], cnt_in.at[ep],
                    s_cnt_s.at[d], s_cnt_r.at[d], {"ep": ep_to(d)})

    load_aff.wait()
    aff_t = jnp.transpose(aff[...])
    for e in range(n_exp):
        at = pl.ds(e * group, group)
        onehot[at, :] = onehot[at, :] * aff_t[:, e:e + 1]
    weight = jnp.transpose(onehot[...])
    high = weight.astype(BF16)
    weight_hi[...] = high
    weight_lo[...] = (weight - high.astype(F32)).astype(BF16)

    for copy in load_w:
        copy.wait()

    for d in ep_order:
        cnt_copy[d].wait_recv()
    lane = lax.broadcasted_iota(jnp.int32, (group, live), 1).astype(F32)
    row = lax.broadcasted_iota(jnp.int32, (group, live), 0).astype(F32)
    start = jnp.zeros((group, live), F32)
    pieces = []
    for j in range(n_ep):
        n = jnp.broadcast_to(cnt_in[j, 0:1, 0:1], (group, live))
        pieces.append(jnp.where((lane - row == start) & (row < n), 1.0, 0.0))
        start = start + n
    spread = jnp.concatenate(pieces, axis=0)
    expand[...] = spread.astype(BF16)
    compact[...] = jnp.transpose(spread).astype(BF16)

    acc[...] = jnp.zeros_like(acc)
    x_copy = {}

    def take(c, k):
        acc[...] += jnp.dot(rows[c, k], wgu[k, c], preferred_element_type=F32)

    def arrivals(c):
        for o in near:
            x_copy[c, o].wait_recv()
            take(c, tp_from(o))

    for c in range(chunks):
        for d in ep_order:
            z_copy[c, d].wait_recv()
        rows[c, tp] = jnp.dot(
            compact[...], z_in[c], preferred_element_type=F32).astype(BF16)
        for o in far:
            x_copy[c, o] = send(
                rows.at[c, tp], rows.at[c, tp],
                s_x_s.at[c, tp_sem(o)], s_x_r.at[c, tp_sem(o)], {"tp": tp_to(o)})
        take(c, tp)
        if c > 0:
            arrivals(c - 1)
    arrivals(chunks - 1)

    gate = acc[:, :hidden]
    up = acc[:, hidden:]
    hid[...] = (gate / (1.0 + jnp.exp(-gate)) * up).astype(BF16)

    for copy in load_d:
        copy.wait()

    p_copy = {}
    for c in range(chunks):
        for o in far + [(0, 0)]:
            k = tp_to(o)
            part_out[c, k] = jnp.dot(
                hid[...], wd[k, :, c * fc:(c + 1) * fc], preferred_element_type=F32
            ).astype(BF16)
            if o != (0, 0):
                p_copy[c, o] = send(
                    part_out.at[c, k], part_in.at[c, tp],
                    s_p_s.at[c, tp_sem(o)], s_p_r.at[c, tp_sem(o)], {"tp": k})

    r_copy = {}
    for c in range(chunks):
        total = part_out[c, tp].astype(F32)
        for o in near:
            p_copy[c, o].wait_recv()
            total = total + part_in[c, tp_from(o)].astype(F32)
        ret_out[c] = jnp.dot(
            expand[...], total.astype(BF16), preferred_element_type=F32).astype(BF16)
        for d in ep_order:
            r_copy[c, d] = send(
                ret_out.at[c, rows_of(ep_to(d)), :], ret_in.at[c, rows_of(ep), :],
                s_r_s.at[c, d], s_r_r.at[c, d], {"ep": ep_to(d)})
        ret_in[c, rows_of(ep), :] = ret_out[c, rows_of(ep), :]

    for c in range(chunks):
        for d in ep_order:
            r_copy[c, d].wait_recv()
        back = ret_in[c]
        out_ref[:, c * fc:(c + 1) * fc] = (
            jnp.dot(weight_hi[...], back, preferred_element_type=F32)
            + jnp.dot(weight_lo[...], back, preferred_element_type=F32)
        ).astype(BF16)

    for copy in sent:
        copy.wait_send()


def per_device(tokens, selected, affinity, w_gate, w_up, w_down):
    n_ep = lax.axis_size("ep")
    n_tp = lax.axis_size("tp")
    n_tok, width = tokens.shape
    n_exp, group = selected.shape
    hidden = w_gate.shape[2]
    assert w_gate.shape[0] == 1 and n_exp == n_ep
    feats = width // n_tp
    chunks = max(1, feats // CHUNK)
    fc = feats // chunks
    slots = n_ep * group
    live = slots // 2
    dma = pltpu.SemaphoreType.DMA
    any_spec = pl.BlockSpec(memory_space=pl.ANY)
    return pl.pallas_call(
        functools.partial(kernel, n_ep, n_tp, chunks),
        out_shape=jax.ShapeDtypeStruct((n_tok, feats), BF16),
        in_specs=[any_spec] * 6,
        out_specs=pl.BlockSpec(memory_space=pltpu.VMEM),
        scratch_shapes=[
            pltpu.VMEM((n_tok, feats), BF16),
            pltpu.VMEM((n_exp, group), jnp.int32),
            pltpu.VMEM((n_exp, group), F32),
            pltpu.VMEM((n_tp, chunks, fc, 2 * hidden), BF16),
            pltpu.VMEM((n_tp, hidden, feats), BF16),
            pltpu.VMEM((slots, n_tok), F32),
            pltpu.VMEM((n_tok, slots), BF16),
            pltpu.VMEM((n_tok, slots), BF16),
            pltpu.VMEM((slots, live), BF16),
            pltpu.VMEM((live, slots), BF16),
            pltpu.VMEM((n_exp, 8, 128), F32),
            pltpu.VMEM((n_ep, 8, 128), F32),
            pltpu.VMEM((chunks, slots, fc), BF16),
            pltpu.VMEM((chunks, slots, fc), BF16),
            pltpu.VMEM((chunks, n_tp, live, fc), BF16),
            pltpu.VMEM((live, 2 * hidden), F32),
            pltpu.VMEM((live, hidden), BF16),
            pltpu.VMEM((chunks, n_tp, live, fc), BF16),
            pltpu.VMEM((chunks, n_tp, live, fc), BF16),
            pltpu.VMEM((chunks, slots, fc), BF16),
            pltpu.VMEM((chunks, slots, fc), BF16),
            dma((3,)),
            dma((n_tp, chunks)),
            dma((n_tp, chunks)),
            dma((n_tp,)),
            dma((n_ep,)),
            dma((n_ep,)),
            dma((chunks, n_ep)),
            dma((chunks, n_ep)),
            dma((chunks, n_tp)),
            dma((chunks, n_tp)),
            dma((chunks, n_tp)),
            dma((chunks, n_tp)),
            dma((chunks, n_ep)),
            dma((chunks, n_ep)),
        ],
        compiler_params=pltpu.CompilerParams(collective_id=0, has_side_effects=True),
    )(tokens, selected, affinity, w_gate, w_up, w_down)


def solution(mesh):
    placed = (
        P("ep", None),
        P(None, "ep"),
        P(None, "ep"),
        P("ep", None, "tp"),
        P("ep", None, "tp"),
        P("ep", "tp", None),
    )
    return jax.shard_map(
        per_device, mesh=mesh, in_specs=placed, out_specs=P("ep", "tp"), check_vma=False
    )
```

```python
import functools
import math

import jax
import jax.numpy as jnp
from jax import lax
from jax.experimental import pallas as pl
from jax.experimental.pallas import tpu as pltpu
from jax.sharding import PartitionSpec as P

MESH = pl.DeviceIdType.MESH
F32 = jnp.float32
BF16 = jnp.bfloat16
CHUNK = 128
LAG = 2


def side_of(n):
    s = math.isqrt(n)
    while n % s:
        s -= 1
    return s


def kernel(
    n_ep, n_tp, chunks,
    tok_hbm, sel_hbm, aff_hbm, wg_hbm, wu_hbm, wd_hbm, out_ref,
    tok, sel, aff, wgu, wd, onehot, weight_hi, weight_lo, expand, compact,
    cnt_out, cnt_in, z_out, z_in, rows, acc, hid, part_out, part_in, ret_out, ret_in,
    s_in, s_wg, s_wu, s_wd, s_cnt_s, s_cnt_r, s_z_s, s_z_r, s_x_s, s_x_r,
    s_p_s, s_p_r, s_r_s, s_r_r,
):
    ep = lax.axis_index("ep")
    tp = lax.axis_index("tp")
    n_tok, feats = tok.shape
    n_exp, group = sel.shape
    fc = feats // chunks
    live = rows.shape[2]
    hidden = hid.shape[1]

    width = side_of(n_tp)
    height = n_tp // width
    y, x = tp // width, lax.rem(tp, width)
    offsets = [(dy, dx) for dy in range(height) for dx in range(width)][1:]
    near = sorted(offsets, key=lambda o: (o[0] > 0) + (o[1] > 0))
    far = near[::-1]

    def tp_to(o):
        return lax.rem(y + o[0], height) * width + lax.rem(x + o[1], width)

    def tp_from(o):
        return lax.rem(y + height - o[0], height) * width + lax.rem(x + width - o[1], width)

    def tp_sem(o):
        return o[0] * width + o[1]

    ep_order = list(range(n_ep - 1))
    high_half = ep // (n_ep // 2)

    def ep_to(i):
        down = n_ep - 1 - i
        down = down - jnp.where(down <= ep, 1, 0)
        up = i + jnp.where(i >= ep, 1, 0)
        return jnp.where(high_half > 0, up, down)

    def ep_from(i):
        return lax.rem(ep + 1 + i, n_ep)

    def rows_of(i):
        return pl.ds(pl.multiple_of(i * group, group), group)

    load_sel = pltpu.make_async_copy(sel_hbm, sel, s_in.at[0])
    load_tok = pltpu.make_async_copy(
        tok_hbm.at[:, pl.ds(pl.multiple_of(tp * feats, 128), feats)], tok, s_in.at[1]
    )
    load_aff = pltpu.make_async_copy(aff_hbm, aff, s_in.at[2])
    load_sel.start()
    load_tok.start()

    barrier = pltpu.get_barrier_semaphore()
    for d in ep_order:
        pl.semaphore_signal(barrier, inc=1, device_id={"ep": ep_to(d)}, device_id_type=MESH)
    for o in far:
        pl.semaphore_signal(barrier, inc=1, device_id={"tp": tp_to(o)}, device_id_type=MESH)

    load_aff.start()
    load_w = []
    for k in range(n_tp):
        for c in range(chunks):
            at = pl.ds(k * feats + c * fc, fc)
            load_w.append(pltpu.make_async_copy(
                wg_hbm.at[0, at, :], wgu.at[k, c, :, pl.ds(0, hidden)], s_wg.at[k, c]))
            load_w.append(pltpu.make_async_copy(
                wu_hbm.at[0, at, :], wgu.at[k, c, :, pl.ds(hidden, hidden)], s_wu.at[k, c]))
    load_d = [
        pltpu.make_async_copy(
            wd_hbm.at[0, :, pl.ds(k * feats, feats)], wd.at[k], s_wd.at[k])
        for k in range(n_tp)
    ]
    for copy in load_w + load_d:
        copy.start()

    load_sel.wait()
    picked = sel[...].astype(F32)
    count = jnp.sum(jnp.where(picked >= 0, 1.0, 0.0), axis=1, keepdims=True)
    for e in range(n_exp):
        cnt_out[e] = jnp.broadcast_to(count[e:e + 1, :], (8, 128))
    picked_t = jnp.transpose(picked)
    token_lane = lax.broadcasted_iota(jnp.int32, (group, n_tok), 1).astype(F32)
    for e in range(n_exp):
        onehot[pl.ds(e * group, group), :] = jnp.where(
            picked_t[:, e:e + 1] == token_lane, 1.0, 0.0)
    load_tok.wait()
    pick = onehot[...].astype(BF16)
    for c in range(chunks):
        z_out[c] = jnp.dot(
            pick, tok[:, c * fc:(c + 1) * fc], preferred_element_type=F32).astype(BF16)
        z_in[c, rows_of(ep), :] = z_out[c, rows_of(ep), :]
    cnt_in[ep] = cnt_out[ep]

    pl.semaphore_wait(barrier, len(ep_order) + len(far))

    sent = []

    def send(src, dst, ss, rs, to):
        copy = pltpu.make_async_remote_copy(
            src_ref=src, dst_ref=dst, send_sem=ss, recv_sem=rs,
            device_id=to, device_id_type=MESH)
        copy.start()
        sent.append(copy)
        return copy

    def arrived(dst, rs):
        pltpu.make_async_remote_copy(
            src_ref=dst, dst_ref=dst, send_sem=s_in.at[0], recv_sem=rs,
            device_id={"ep": ep_from(0)}, device_id_type=MESH).wait_recv()

    for c in range(chunks):
        for d in ep_order:
            send(
                z_out.at[c, rows_of(ep_to(d)), :], z_in.at[c, rows_of(ep), :],
                s_z_s.at[c, d], s_z_r.at[c, ep], {"ep": ep_to(d)})
            if c == 0:
                send(
                    cnt_out.at[ep_to(d)], cnt_in.at[ep],
                    s_cnt_s.at[d], s_cnt_r.at[ep], {"ep": ep_to(d)})

    load_aff.wait()
    aff_t = jnp.transpose(aff[...])
    for e in range(n_exp):
        at = pl.ds(e * group, group)
        onehot[at, :] = onehot[at, :] * aff_t[:, e:e + 1]
    weight = jnp.transpose(onehot[...])
    high = weight.astype(BF16)
    weight_hi[...] = high
    weight_lo[...] = (weight - high.astype(F32)).astype(BF16)

    for copy in load_w:
        copy.wait()

    for d in ep_order:
        arrived(cnt_in.at[ep_from(d)], s_cnt_r.at[ep_from(d)])
    lane = lax.broadcasted_iota(jnp.int32, (group, live), 1).astype(F32)
    row = lax.broadcasted_iota(jnp.int32, (group, live), 0).astype(F32)
    start = jnp.zeros((group, live), F32)
    pieces = []
    for j in range(n_ep):
        n = jnp.broadcast_to(cnt_in[j, 0:1, 0:1], (group, live))
        pieces.append(jnp.where((lane - row == start) & (row < n), 1.0, 0.0))
        start = start + n
    spread = jnp.concatenate(pieces, axis=0)
    expand[...] = spread.astype(BF16)
    compact[...] = jnp.transpose(spread).astype(BF16)

    acc[...] = jnp.zeros_like(acc)
    x_copy = {}

    def take(c, k):
        acc[...] += jnp.dot(rows[c, k], wgu[k, c], preferred_element_type=F32)

    def arrivals(c):
        for o in near:
            x_copy[c, o].wait_recv()
            take(c, tp_from(o))

    for c in range(chunks):
        for d in ep_order:
            arrived(z_in.at[c, rows_of(ep_from(d)), :], s_z_r.at[c, ep_from(d)])
        rows[c, tp] = jnp.dot(
            compact[...], z_in[c], preferred_element_type=F32).astype(BF16)
        for o in far:
            x_copy[c, o] = send(
                rows.at[c, tp], rows.at[c, tp],
                s_x_s.at[c, tp_sem(o)], s_x_r.at[c, tp_sem(o)], {"tp": tp_to(o)})
        take(c, tp)
        if c >= LAG:
            arrivals(c - LAG)
    for c in range(max(0, chunks - LAG), chunks):
        arrivals(c)

    gate = acc[:, :hidden]
    up = acc[:, hidden:]
    hid[...] = (gate / (1.0 + jnp.exp(-gate)) * up).astype(BF16)

    for copy in load_d:
        copy.wait()

    p_copy = {}
    for c in range(chunks):
        for o in far + [(0, 0)]:
            k = tp_to(o)
            part_out[c, k] = jnp.dot(
                hid[...], wd[k, :, c * fc:(c + 1) * fc], preferred_element_type=F32
            ).astype(BF16)
            if o != (0, 0):
                p_copy[c, o] = send(
                    part_out.at[c, k], part_in.at[c, tp],
                    s_p_s.at[c, tp_sem(o)], s_p_r.at[c, tp_sem(o)], {"tp": k})

    for c in range(chunks):
        total = part_out[c, tp].astype(F32)
        for o in near:
            p_copy[c, o].wait_recv()
            total = total + part_in[c, tp_from(o)].astype(F32)
        ret_out[c] = jnp.dot(
            expand[...], total.astype(BF16), preferred_element_type=F32).astype(BF16)
        for d in ep_order:
            send(
                ret_out.at[c, rows_of(ep_to(d)), :], ret_in.at[c, rows_of(ep), :],
                s_r_s.at[c, d], s_r_r.at[c, ep], {"ep": ep_to(d)})
        ret_in[c, rows_of(ep), :] = ret_out[c, rows_of(ep), :]

    for c in range(chunks):
        for d in ep_order:
            arrived(ret_in.at[c, rows_of(ep_from(d)), :], s_r_r.at[c, ep_from(d)])
        back = ret_in[c]
        out_ref[:, c * fc:(c + 1) * fc] = (
            jnp.dot(weight_hi[...], back, preferred_element_type=F32)
            + jnp.dot(weight_lo[...], back, preferred_element_type=F32)
        ).astype(BF16)

    for copy in sent:
        copy.wait_send()


def per_device(tokens, selected, affinity, w_gate, w_up, w_down):
    n_ep = lax.axis_size("ep")
    n_tp = lax.axis_size("tp")
    n_tok, width = tokens.shape
    n_exp, group = selected.shape
    hidden = w_gate.shape[2]
    assert w_gate.shape[0] == 1 and n_exp == n_ep
    feats = width // n_tp
    chunks = max(1, feats // CHUNK)
    fc = feats // chunks
    slots = n_ep * group
    live = slots // 2
    dma = pltpu.SemaphoreType.DMA
    any_spec = pl.BlockSpec(memory_space=pl.ANY)
    return pl.pallas_call(
        functools.partial(kernel, n_ep, n_tp, chunks),
        out_shape=pltpu.VMEM((n_tok, feats), BF16),
        in_specs=[any_spec] * 6,
        out_specs=pl.BlockSpec(memory_space=pltpu.VMEM),
        scratch_shapes=[
            pltpu.VMEM((n_tok, feats), BF16),
            pltpu.VMEM((n_exp, group), jnp.int32),
            pltpu.VMEM((n_exp, group), F32),
            pltpu.VMEM((n_tp, chunks, fc, 2 * hidden), BF16),
            pltpu.VMEM((n_tp, hidden, feats), BF16),
            pltpu.VMEM((slots, n_tok), F32),
            pltpu.VMEM((n_tok, slots), BF16),
            pltpu.VMEM((n_tok, slots), BF16),
            pltpu.VMEM((slots, live), BF16),
            pltpu.VMEM((live, slots), BF16),
            pltpu.VMEM((n_exp, 8, 128), F32),
            pltpu.VMEM((n_ep, 8, 128), F32),
            pltpu.VMEM((chunks, slots, fc), BF16),
            pltpu.VMEM((chunks, slots, fc), BF16),
            pltpu.VMEM((chunks, n_tp, live, fc), BF16),
            pltpu.VMEM((live, 2 * hidden), F32),
            pltpu.VMEM((live, hidden), BF16),
            pltpu.VMEM((chunks, n_tp, live, fc), BF16),
            pltpu.VMEM((chunks, n_tp, live, fc), BF16),
            pltpu.VMEM((chunks, slots, fc), BF16),
            pltpu.VMEM((chunks, slots, fc), BF16),
            dma((3,)),
            dma((n_tp, chunks)),
            dma((n_tp, chunks)),
            dma((n_tp,)),
            dma((n_ep,)),
            dma((n_ep,)),
            dma((chunks, n_ep)),
            dma((chunks, n_ep)),
            dma((chunks, n_tp)),
            dma((chunks, n_tp)),
            dma((chunks, n_tp)),
            dma((chunks, n_tp)),
            dma((chunks, n_ep)),
            dma((chunks, n_ep)),
        ],
        compiler_params=pltpu.CompilerParams(collective_id=0, has_side_effects=True),
    )(tokens, selected, affinity, w_gate, w_up, w_down)


def solution(mesh):
    placed = (
        P("ep", None),
        P(None, "ep"),
        P(None, "ep"),
        P("ep", None, "tp"),
        P("ep", None, "tp"),
        P("ep", "tp", None),
    )
    return jax.shard_map(
        per_device, mesh=mesh, in_specs=placed, out_specs=P("ep", "tp"), check_vma=False
    )
```

```python
import functools
import math

import jax
import jax.numpy as jnp
from jax import lax
from jax.experimental import pallas as pl
from jax.experimental.pallas import tpu as pltpu
from jax.sharding import PartitionSpec as P

MESH = pl.DeviceIdType.MESH
F32 = jnp.float32
BF16 = jnp.bfloat16
CHUNK = 128
LAG = 2


def side_of(n):
    s = math.isqrt(n)
    while n % s:
        s -= 1
    return s


def kernel(
    n_ep, n_tp, chunks,
    tok_hbm, sel_hbm, aff_hbm, wg_hbm, wu_hbm, wd_hbm, out_ref,
    tok, sel, aff, wgu, wd, onehot, weight_hi, weight_lo, expand, compact,
    cnt_out, cnt_in, z_out, z_in, rows, acc, hid, part_out, part_in, ret_out, ret_in,
    s_in, s_w, s_cnt_s, s_cnt_r, s_z_s, s_z_r, s_x_s, s_x_r,
    s_p_s, s_p_r, s_r_s, s_r_r,
):
    ep = lax.axis_index("ep")
    tp = lax.axis_index("tp")
    n_tok, feats = tok.shape
    n_exp, group = sel.shape
    fc = feats // chunks
    live = rows.shape[2]
    hidden = hid.shape[1]

    width = side_of(n_tp)
    height = n_tp // width
    y, x = tp // width, lax.rem(tp, width)
    offsets = [(dy, dx) for dy in range(height) for dx in range(width)][1:]
    near = sorted(offsets, key=lambda o: (o[0] > 0) + (o[1] > 0))
    far = near[::-1]

    def tp_to(o):
        return lax.rem(y + o[0], height) * width + lax.rem(x + o[1], width)

    def tp_from(o):
        return lax.rem(y + height - o[0], height) * width + lax.rem(x + width - o[1], width)

    def tp_sem(o):
        return o[0] * width + o[1]

    ep_order = list(range(n_ep - 1))
    high_half = ep // (n_ep // 2)

    def ep_to(i):
        down = n_ep - 1 - i
        down = down - jnp.where(down <= ep, 1, 0)
        up = i + jnp.where(i >= ep, 1, 0)
        return jnp.where(high_half > 0, up, down)

    def rows_of(i):
        return pl.ds(pl.multiple_of(i * group, group), group)

    def cols(k, c):
        return pl.ds(pl.multiple_of(k * feats + c * fc, 128), fc)

    load_sel = pltpu.make_async_copy(sel_hbm, sel, s_in.at[0])
    load_tok = pltpu.make_async_copy(
        tok_hbm.at[:, pl.ds(pl.multiple_of(tp * feats, 128), feats)], tok, s_in.at[1]
    )
    load_aff = pltpu.make_async_copy(aff_hbm, aff, s_in.at[2])
    load_sel.start()
    load_tok.start()

    barrier = pltpu.get_barrier_semaphore()
    for d in ep_order:
        pl.semaphore_signal(barrier, inc=1, device_id={"ep": ep_to(d)}, device_id_type=MESH)
    for o in far:
        pl.semaphore_signal(barrier, inc=1, device_id={"tp": tp_to(o)}, device_id_type=MESH)

    load_aff.start()

    load_sel.wait()
    picked = sel[...].astype(F32)
    count = jnp.sum(jnp.where(picked >= 0, 1.0, 0.0), axis=1, keepdims=True)
    for e in range(n_exp):
        cnt_out[e] = jnp.broadcast_to(count[e:e + 1, :], (1, 128))
    picked_t = jnp.transpose(picked)
    token_lane = lax.broadcasted_iota(jnp.int32, (group, n_tok), 1).astype(F32)
    for e in range(n_exp):
        onehot[pl.ds(e * group, group), :] = jnp.where(
            picked_t[:, e:e + 1] == token_lane, 1.0, 0.0)
    load_tok.wait()
    pick = onehot[...].astype(BF16)
    for c in range(chunks):
        z_out[c] = jnp.dot(
            pick, tok[:, c * fc:(c + 1) * fc], preferred_element_type=F32).astype(BF16)
        z_in[c, rows_of(ep), :] = z_out[c, rows_of(ep), :]
    cnt_in[ep] = cnt_out[ep]

    pl.semaphore_wait(barrier, len(ep_order) + len(far))


    def send(src, dst, ss, rs, to):
        copy = pltpu.make_async_remote_copy(
            src_ref=src, dst_ref=dst, send_sem=ss, recv_sem=rs,
            device_id=to, device_id_type=MESH)
        copy.start()
        return copy

    others = (n_ep - 1) * group

    def whole(ref, ss, rs):
        return pltpu.make_async_remote_copy(
            src_ref=ref, dst_ref=ref, send_sem=ss, recv_sem=rs,
            device_id={"ep": ep_to(0)}, device_id_type=MESH)

    cnt_all = whole(cnt_in.at[pl.ds(0, n_ep - 1)], s_cnt_s.at[0], s_cnt_r.at[0])
    z_all = [
        whole(z_in.at[c, pl.ds(0, others), :], s_z_s.at[c], s_z_r.at[c]) for c in range(chunks)]
    r_all = [
        whole(ret_in.at[c, pl.ds(0, others), :], s_r_s.at[c], s_r_r.at[c]) for c in range(chunks)]

    for c in range(chunks):
        for d in ep_order:
            send(
                z_out.at[c, rows_of(ep_to(d)), :], z_in.at[c, rows_of(ep), :],
                s_z_s.at[c], s_z_r.at[c], {"ep": ep_to(d)})
            if c == 0:
                send(
                    cnt_out.at[ep_to(d)], cnt_in.at[ep],
                    s_cnt_s.at[0], s_cnt_r.at[0], {"ep": ep_to(d)})

    load_w = [
        pltpu.make_async_copy(wg_hbm.at[0], wgu.at[:, pl.ds(0, hidden)], s_w.at[0]),
        pltpu.make_async_copy(wu_hbm.at[0], wgu.at[:, pl.ds(hidden, hidden)], s_w.at[1]),
    ]
    load_d = [pltpu.make_async_copy(wd_hbm.at[0], wd, s_w.at[2])]
    for copy in load_w + load_d:
        copy.start()

    load_aff.wait()
    aff_t = jnp.transpose(aff[...])
    for e in range(n_exp):
        at = pl.ds(e * group, group)
        onehot[at, :] = onehot[at, :] * aff_t[:, e:e + 1]
    weight = jnp.transpose(onehot[...])
    high = weight.astype(BF16)
    weight_hi[...] = high
    weight_lo[...] = (weight - high.astype(F32)).astype(BF16)

    for copy in load_w:
        copy.wait()

    cnt_all.wait_recv()
    lane = lax.broadcasted_iota(jnp.int32, (group, live), 1).astype(F32)
    row = lax.broadcasted_iota(jnp.int32, (group, live), 0).astype(F32)
    start = jnp.zeros((group, live), F32)
    pieces = []
    for j in range(n_ep):
        n = jnp.broadcast_to(cnt_in[j, 0:1, 0:1], (group, live))
        pieces.append(jnp.where((lane - row == start) & (row < n), 1.0, 0.0))
        start = start + n
    spread = jnp.concatenate(pieces, axis=0)
    expand[...] = spread.astype(BF16)
    compact[...] = jnp.transpose(spread).astype(BF16)

    acc[...] = jnp.zeros_like(acc)
    x_copy = {}

    def take(c, k):
        acc[...] += jnp.dot(rows[c, k], wgu[cols(k, c), :], preferred_element_type=F32)

    def arrivals(c):
        for o in near:
            x_copy[c, o].wait_recv()
            take(c, tp_from(o))

    for c in range(chunks):
        z_all[c].wait_recv()
        rows[c, tp] = jnp.dot(
            compact[...], z_in[c], preferred_element_type=F32).astype(BF16)
        for o in far:
            x_copy[c, o] = send(
                rows.at[c, tp], rows.at[c, tp],
                s_x_s.at[c, tp_sem(o)], s_x_r.at[c, tp_sem(o)], {"tp": tp_to(o)})
        take(c, tp)
        if c >= LAG:
            arrivals(c - LAG)
    for c in range(max(0, chunks - LAG), chunks):
        arrivals(c)

    gate = acc[:, :hidden]
    up = acc[:, hidden:]
    hid[...] = (gate / (1.0 + jnp.exp(-gate)) * up).astype(BF16)

    for copy in load_d:
        copy.wait()

    p_copy = {}
    for c in range(chunks):
        for o in far + [(0, 0)]:
            k = tp_to(o)
            part_out[c, k] = jnp.dot(
                hid[...], wd[:, cols(k, c)], preferred_element_type=F32
            ).astype(BF16)
            if o != (0, 0):
                p_copy[c, o] = send(
                    part_out.at[c, k], part_in.at[c, tp],
                    s_p_s.at[c, tp_sem(o)], s_p_r.at[c, tp_sem(o)], {"tp": k})

    for c in range(chunks):
        total = part_out[c, tp].astype(F32)
        for o in near:
            p_copy[c, o].wait_recv()
            total = total + part_in[c, tp_from(o)].astype(F32)
        ret_out[c] = jnp.dot(
            expand[...], total.astype(BF16), preferred_element_type=F32).astype(BF16)
        for d in ep_order:
            send(
                ret_out.at[c, rows_of(ep_to(d)), :], ret_in.at[c, rows_of(ep), :],
                s_r_s.at[c], s_r_r.at[c], {"ep": ep_to(d)})
        ret_in[c, rows_of(ep), :] = ret_out[c, rows_of(ep), :]

    for copy in [cnt_all] + z_all + list(x_copy.values()) + list(p_copy.values()):
        copy.wait_send()

    for c in range(chunks):
        r_all[c].wait_recv()
        back = ret_in[c]
        out_ref[:, c * fc:(c + 1) * fc] = (
            jnp.dot(weight_hi[...], back, preferred_element_type=F32)
            + jnp.dot(weight_lo[...], back, preferred_element_type=F32)
        ).astype(BF16)

    for copy in r_all:
        copy.wait_send()


def per_device(tokens, selected, affinity, w_gate, w_up, w_down):
    n_ep = lax.axis_size("ep")
    n_tp = lax.axis_size("tp")
    n_tok, width = tokens.shape
    n_exp, group = selected.shape
    hidden = w_gate.shape[2]
    assert w_gate.shape[0] == 1 and n_exp == n_ep
    feats = width // n_tp
    chunks = max(1, feats // CHUNK)
    fc = feats // chunks
    slots = n_ep * group
    live = slots // 2
    dma = pltpu.SemaphoreType.DMA
    any_spec = pl.BlockSpec(memory_space=pl.ANY)
    return pl.pallas_call(
        functools.partial(kernel, n_ep, n_tp, chunks),
        out_shape=pltpu.VMEM((n_tok, feats), BF16),
        in_specs=[any_spec] * 6,
        out_specs=pl.BlockSpec(memory_space=pltpu.VMEM),
        scratch_shapes=[
            pltpu.VMEM((n_tok, feats), BF16),
            pltpu.VMEM((n_exp, group), jnp.int32),
            pltpu.VMEM((n_exp, group), F32),
            pltpu.VMEM((width, 2 * hidden), BF16),
            pltpu.VMEM((hidden, width), BF16),
            pltpu.VMEM((slots, n_tok), F32),
            pltpu.VMEM((n_tok, slots), BF16),
            pltpu.VMEM((n_tok, slots), BF16),
            pltpu.VMEM((slots, live), BF16),
            pltpu.VMEM((live, slots), BF16),
            pltpu.VMEM((n_exp, 1, 128), F32),
            pltpu.VMEM((n_ep, 1, 128), F32),
            pltpu.VMEM((chunks, slots, fc), BF16),
            pltpu.VMEM((chunks, slots, fc), BF16),
            pltpu.VMEM((chunks, n_tp, live, fc), BF16),
            pltpu.VMEM((live, 2 * hidden), F32),
            pltpu.VMEM((live, hidden), BF16),
            pltpu.VMEM((chunks, n_tp, live, fc), BF16),
            pltpu.VMEM((chunks, n_tp, live, fc), BF16),
            pltpu.VMEM((chunks, slots, fc), BF16),
            pltpu.VMEM((chunks, slots, fc), BF16),
            dma((3,)),
            dma((3,)),
            dma((1,)),
            dma((1,)),
            dma((chunks,)),
            dma((chunks,)),
            dma((chunks, n_tp)),
            dma((chunks, n_tp)),
            dma((chunks, n_tp)),
            dma((chunks, n_tp)),
            dma((chunks,)),
            dma((chunks,)),
        ],
        compiler_params=pltpu.CompilerParams(collective_id=0, has_side_effects=True),
    )(tokens, selected, affinity, w_gate, w_up, w_down)


def solution(mesh):
    placed = (
        P("ep", None),
        P(None, "ep"),
        P(None, "ep"),
        P("ep", None, "tp"),
        P("ep", None, "tp"),
        P("ep", "tp", None),
    )
    return jax.shard_map(
        per_device, mesh=mesh, in_specs=placed, out_specs=P("ep", "tp"), check_vma=False
    )
```

```python
import functools
import math

import jax
import jax.numpy as jnp
from jax import lax
from jax.experimental import pallas as pl
from jax.experimental.pallas import tpu as pltpu
from jax.sharding import PartitionSpec as P

MESH = pl.DeviceIdType.MESH
F32 = jnp.float32
BF16 = jnp.bfloat16
CHUNK = 128
LAG = 2


def side_of(n):
    s = math.isqrt(n)
    while n % s:
        s -= 1
    return s


def kernel(
    n_ep, n_tp, chunks,
    tok_hbm, sel_hbm, aff_hbm, wg_hbm, wu_hbm, wd_hbm, out_ref,
    tok, sel, aff, wgu, wd, onehot, weight_hi, weight_lo, expand, compact,
    cnt_out, cnt_in, z_out, z_in, rows, acc, hid, part_out, part_in, ret_out, ret_in,
    s_in, s_w, s_cnt_s, s_cnt_r, s_z_s, s_z_r, s_x_s, s_x_r,
    s_p_s, s_p_r, s_r_s, s_r_r,
):
    ep = lax.axis_index("ep")
    tp = lax.axis_index("tp")
    n_tok, feats = tok.shape
    n_exp, group = sel.shape
    fc = feats // chunks
    live = rows.shape[2]
    hidden = hid.shape[1]

    width = side_of(n_tp)
    height = n_tp // width
    y, x = tp // width, lax.rem(tp, width)
    offsets = [(dy, dx) for dy in range(height) for dx in range(width)][1:]
    near = sorted(offsets, key=lambda o: (o[0] > 0) + (o[1] > 0))
    far = near[::-1]

    def tp_to(o):
        return lax.rem(y + o[0], height) * width + lax.rem(x + o[1], width)

    def tp_from(o):
        return lax.rem(y + height - o[0], height) * width + lax.rem(x + width - o[1], width)

    def tp_sem(o):
        return o[0] * width + o[1]

    ep_order = list(range(n_ep - 1))
    high_half = ep // (n_ep // 2)

    def ep_to(i):
        down = n_ep - 1 - i
        down = down - jnp.where(down <= ep, 1, 0)
        up = i + jnp.where(i >= ep, 1, 0)
        return jnp.where(high_half > 0, up, down)

    def rows_of(i):
        return pl.ds(pl.multiple_of(i * group, group), group)

    def cols(k, c):
        return pl.ds(pl.multiple_of(k * feats + c * fc, 128), fc)

    load_sel = pltpu.make_async_copy(sel_hbm, sel, s_in.at[0])
    load_tok = pltpu.make_async_copy(
        tok_hbm.at[:, pl.ds(pl.multiple_of(tp * feats, 128), feats)], tok, s_in.at[1]
    )
    load_aff = pltpu.make_async_copy(aff_hbm, aff, s_in.at[2])
    load_sel.start()
    load_tok.start()

    barrier = pltpu.get_barrier_semaphore()
    for d in ep_order:
        pl.semaphore_signal(barrier, inc=1, device_id={"ep": ep_to(d)}, device_id_type=MESH)
    for o in far:
        pl.semaphore_signal(barrier, inc=1, device_id={"tp": tp_to(o)}, device_id_type=MESH)

    load_aff.start()

    load_sel.wait()
    picked = sel[...].astype(F32)
    count = jnp.sum(jnp.where(picked >= 0, 1.0, 0.0), axis=1, keepdims=True)
    for e in range(n_exp):
        cnt_out[e] = jnp.broadcast_to(count[e:e + 1, :], (1, 128))
    picked_t = jnp.transpose(picked)
    token_lane = lax.broadcasted_iota(jnp.int32, (group, n_tok), 1).astype(F32)
    for e in range(n_exp):
        onehot[pl.ds(e * group, group), :] = jnp.where(
            picked_t[:, e:e + 1] == token_lane, 1.0, 0.0)
    load_tok.wait()
    pick = onehot[...].astype(BF16)
    for c in range(chunks):
        z_out[c] = jnp.dot(
            pick, tok[:, c * fc:(c + 1) * fc], preferred_element_type=F32).astype(BF16)
        z_in[c, rows_of(ep), :] = z_out[c, rows_of(ep), :]
    cnt_in[ep] = cnt_out[ep]

    pl.semaphore_wait(barrier, len(ep_order) + len(far))


    def send(src, dst, ss, rs, to):
        copy = pltpu.make_async_remote_copy(
            src_ref=src, dst_ref=dst, send_sem=ss, recv_sem=rs,
            device_id=to, device_id_type=MESH)
        copy.start()
        return copy

    others = (n_ep - 1) * group

    def whole(ref, ss, rs):
        return pltpu.make_async_remote_copy(
            src_ref=ref, dst_ref=ref, send_sem=ss, recv_sem=rs,
            device_id={"ep": ep_to(0)}, device_id_type=MESH)

    cnt_all = whole(cnt_in.at[pl.ds(0, n_ep - 1)], s_cnt_s.at[0], s_cnt_r.at[0])
    z_all = [
        whole(z_in.at[c, pl.ds(0, others), :], s_z_s.at[c], s_z_r.at[c]) for c in range(chunks)]
    r_all = [
        whole(ret_in.at[c, pl.ds(0, others), :], s_r_s.at[c], s_r_r.at[c]) for c in range(chunks)]

    for c in range(chunks):
        for d in ep_order:
            send(
                z_out.at[c, rows_of(ep_to(d)), :], z_in.at[c, rows_of(ep), :],
                s_z_s.at[c], s_z_r.at[c], {"ep": ep_to(d)})
            if c == 0:
                send(
                    cnt_out.at[ep_to(d)], cnt_in.at[ep],
                    s_cnt_s.at[0], s_cnt_r.at[0], {"ep": ep_to(d)})

    load_w = [
        pltpu.make_async_copy(wg_hbm.at[0], wgu.at[:, pl.ds(0, hidden)], s_w.at[0]),
        pltpu.make_async_copy(wu_hbm.at[0], wgu.at[:, pl.ds(hidden, hidden)], s_w.at[1]),
    ]
    load_d = [pltpu.make_async_copy(wd_hbm.at[0], wd, s_w.at[2])]
    for copy in load_w + load_d:
        copy.start()

    load_aff.wait()
    aff_t = jnp.transpose(aff[...])
    for e in range(n_exp):
        at = pl.ds(e * group, group)
        onehot[at, :] = onehot[at, :] * aff_t[:, e:e + 1]
    weight = jnp.transpose(onehot[...])
    high = weight.astype(BF16)
    weight_hi[...] = high
    weight_lo[...] = (weight - high.astype(F32)).astype(BF16)

    for copy in load_w:
        copy.wait()

    cnt_all.wait_recv()
    lane = lax.broadcasted_iota(jnp.int32, (group, live), 1).astype(F32)
    row = lax.broadcasted_iota(jnp.int32, (group, live), 0).astype(F32)
    start = jnp.zeros((group, live), F32)
    pieces = []
    for j in range(n_ep):
        n = jnp.broadcast_to(cnt_in[j, 0:1, 0:1], (group, live))
        pieces.append(jnp.where((lane - row == start) & (row < n), 1.0, 0.0))
        start = start + n
    spread = jnp.concatenate(pieces, axis=0)
    expand[...] = spread.astype(BF16)
    compact[...] = jnp.transpose(spread).astype(BF16)

    acc[...] = jnp.zeros_like(acc)
    x_copy = {}

    def take(c, k):
        acc[...] += jnp.dot(rows[c, k], wgu[cols(k, c), :], preferred_element_type=F32)

    def arrivals(c):
        for o in near:
            x_copy[c, o].wait_recv()
            take(c, tp_from(o))

    for c in range(chunks):
        z_all[c].wait_recv()
        rows[c, tp] = jnp.dot(
            compact[...], z_in[c], preferred_element_type=F32).astype(BF16)
        for o in near:
            x_copy[c, o] = send(
                rows.at[c, tp], rows.at[c, tp],
                s_x_s.at[c, tp_sem(o)], s_x_r.at[c, tp_sem(o)], {"tp": tp_to(o)})
        take(c, tp)
        if c >= LAG:
            arrivals(c - LAG)
    for c in range(max(0, chunks - LAG), chunks):
        arrivals(c)

    gate = acc[:, :hidden]
    up = acc[:, hidden:]
    hid[...] = (gate / (1.0 + jnp.exp(-gate)) * up).astype(BF16)

    for copy in load_d:
        copy.wait()

    p_copy = {}
    for c in range(chunks):
        for o in near + [(0, 0)]:
            k = tp_to(o)
            part_out[c, k] = jnp.dot(
                hid[...], wd[:, cols(k, c)], preferred_element_type=F32
            ).astype(BF16)
            if o != (0, 0):
                p_copy[c, o] = send(
                    part_out.at[c, k], part_in.at[c, tp],
                    s_p_s.at[c, tp_sem(o)], s_p_r.at[c, tp_sem(o)], {"tp": k})

    for c in range(chunks):
        total = part_out[c, tp].astype(F32)
        for o in near:
            p_copy[c, o].wait_recv()
            total = total + part_in[c, tp_from(o)].astype(F32)
        ret_out[c] = jnp.dot(
            expand[...], total.astype(BF16), preferred_element_type=F32).astype(BF16)
        for d in ep_order:
            send(
                ret_out.at[c, rows_of(ep_to(d)), :], ret_in.at[c, rows_of(ep), :],
                s_r_s.at[c], s_r_r.at[c], {"ep": ep_to(d)})
        ret_in[c, rows_of(ep), :] = ret_out[c, rows_of(ep), :]

    for copy in [cnt_all] + z_all + list(x_copy.values()) + list(p_copy.values()):
        copy.wait_send()

    for c in range(chunks):
        r_all[c].wait_recv()
        back = ret_in[c]
        out_ref[:, c * fc:(c + 1) * fc] = (
            jnp.dot(weight_hi[...], back, preferred_element_type=F32)
            + jnp.dot(weight_lo[...], back, preferred_element_type=F32)
        ).astype(BF16)

    for copy in r_all:
        copy.wait_send()


def per_device(tokens, selected, affinity, w_gate, w_up, w_down):
    n_ep = lax.axis_size("ep")
    n_tp = lax.axis_size("tp")
    n_tok, width = tokens.shape
    n_exp, group = selected.shape
    hidden = w_gate.shape[2]
    assert w_gate.shape[0] == 1 and n_exp == n_ep
    feats = width // n_tp
    chunks = max(1, feats // CHUNK)
    fc = feats // chunks
    slots = n_ep * group
    live = slots // 2
    dma = pltpu.SemaphoreType.DMA
    any_spec = pl.BlockSpec(memory_space=pl.ANY)
    return pl.pallas_call(
        functools.partial(kernel, n_ep, n_tp, chunks),
        out_shape=pltpu.VMEM((n_tok, feats), BF16),
        in_specs=[any_spec] * 6,
        out_specs=pl.BlockSpec(memory_space=pltpu.VMEM),
        scratch_shapes=[
            pltpu.VMEM((n_tok, feats), BF16),
            pltpu.VMEM((n_exp, group), jnp.int32),
            pltpu.VMEM((n_exp, group), F32),
            pltpu.VMEM((width, 2 * hidden), BF16),
            pltpu.VMEM((hidden, width), BF16),
            pltpu.VMEM((slots, n_tok), F32),
            pltpu.VMEM((n_tok, slots), BF16),
            pltpu.VMEM((n_tok, slots), BF16),
            pltpu.VMEM((slots, live), BF16),
            pltpu.VMEM((live, slots), BF16),
            pltpu.VMEM((n_exp, 1, 128), F32),
            pltpu.VMEM((n_ep, 1, 128), F32),
            pltpu.VMEM((chunks, slots, fc), BF16),
            pltpu.VMEM((chunks, slots, fc), BF16),
            pltpu.VMEM((chunks, n_tp, live, fc), BF16),
            pltpu.VMEM((live, 2 * hidden), F32),
            pltpu.VMEM((live, hidden), BF16),
            pltpu.VMEM((chunks, n_tp, live, fc), BF16),
            pltpu.VMEM((chunks, n_tp, live, fc), BF16),
            pltpu.VMEM((chunks, slots, fc), BF16),
            pltpu.VMEM((chunks, slots, fc), BF16),
            dma((3,)),
            dma((3,)),
            dma((1,)),
            dma((1,)),
            dma((chunks,)),
            dma((chunks,)),
            dma((chunks, n_tp)),
            dma((chunks, n_tp)),
            dma((chunks, n_tp)),
            dma((chunks, n_tp)),
            dma((chunks,)),
            dma((chunks,)),
        ],
        compiler_params=pltpu.CompilerParams(collective_id=0, has_side_effects=True),
    )(tokens, selected, affinity, w_gate, w_up, w_down)


def solution(mesh):
    placed = (
        P("ep", None),
        P(None, "ep"),
        P(None, "ep"),
        P("ep", None, "tp"),
        P("ep", None, "tp"),
        P("ep", "tp", None),
    )
    return jax.shard_map(
        per_device, mesh=mesh, in_specs=placed, out_specs=P("ep", "tp"), check_vma=False
    )
```
